32 devices in a mesh: sp: 8 (over z, x), tp: 4 (over y, core).
Axes of the slice: x: 2, y: 2, z: 4, core: 2. Of those that a mesh axis runs over, the one named last changes fastest.
Arguments:
- query_one: bfloat16 [1024, 1024], P('sp', 'tp'), may hold values from -100 to 100
- key_one: bfloat16 [1024, 512], P('sp', 'tp'), may hold values from -10 to 10
- query_two: bfloat16 [1024, 1024], P('sp', 'tp'), may hold values from -100 to 100
- key_two: bfloat16 [1024, 512], P('sp', 'tp'), may hold values from -10 to 10
- value: bfloat16 [1024, 1024], P('sp', 'tp'), may hold values from -6 to 6
- lambda_head: float32 [8], P('tp'), may hold values from 0.3 to 0.8
- head_gain: float32 [256], replicated, may hold values from 0.1 to 1.9
- out_weight: bfloat16 [2048, 4096], P('tp'), may hold values from -0.125 to 0.125
- residual: bfloat16 [1024, 4096], P(('sp', 'tp')), may hold values from -6 to 6
- norm_gain: float32 [4096], replicated, may hold values from 0.1 to 1.9
- route_expert: int32 [1024, 2], P(('sp', 'tp')), may hold values from 0 to 7, all different within a row; in each aligned block of 32 rows (0 to 31, 32 to 63, ...) at most 16 rows name the same one
- route_weight: float32 [1024, 2], P(('sp', 'tp')), may hold values from 0.1 to 0.9
- expert_gate: bfloat16 [8, 4096, 1024], P('sp', None, 'tp'), may hold values from -0.09375 to 0.09375
- expert_up: bfloat16 [8, 4096, 1024], P('sp', None, 'tp'), may hold values from -0.09375 to 0.09375
- expert_down: bfloat16 [8, 1024, 4096], P('sp', 'tp'), may hold values from -0.1875 to 0.1875
Outputs:
- output: bfloat16 [1024, 4096], P(('sp', 'tp'))
The draws below stay inside these ranges and needn't reach their ends.
Inputs may be any that keep to these rules, and one draw needn't show every extreme that they name: `route_expert`: the 2 entries of a row differ. In each aligned block of 32 rows (the rows of one device) no expert is named more than 16 times, a bound that some block reaches.
All inputs are finite; a program needn't handle non-finite values.
Results may differ from the reference program's by a relative error of at most 0.015.
Values may be sent and summed in bfloat16 or wider, within the bound.
No kernel may reach another device: no remote copies, remote signals or barrier semaphores. Data moves between devices by JAX's collectives and lax.ppermute only.
A program may use at most 128 MiB of HBM per device.

```python
import math
import jax
import jax.numpy as jnp
import numpy as np
from jax import lax

D = 4096
HEADS = 8
KV_HEADS = 4
HEAD = 128
EXPERT_FF = 1024
TOP = 2
TOKENS = 1024
ROWS_DEV = 32
EXPERTS = 8
CAP = 16
FF_PART = 256
N_TP = 4


def drawn(key, which):
    folded = jax.random.fold_in(key, which)
    query_key, key_key = jax.random.split(folded)
    key_rows = jnp.clip(1.3 * jax.random.normal(key_key, (TOKENS, KV_HEADS * HEAD), jnp.float32), -7.8, 7.8)
    query_rows = jnp.clip(1.3 * jax.random.normal(query_key, (TOKENS, HEADS * HEAD), jnp.float32), -7.8, 7.8)
    return (query_rows, key_rows)


def draw_query_one(key, part):
    return drawn(key, 11)[0].astype(jnp.bfloat16)


def draw_key_one(key, part):
    return drawn(key, 11)[1].astype(jnp.bfloat16)


def draw_query_two(key, part):
    return drawn(key, 23)[0].astype(jnp.bfloat16)


def draw_key_two(key, part):
    return drawn(key, 23)[1].astype(jnp.bfloat16)


def levels(rng, shape, shards, low, high):
    factor_of, own = 1.0, jax.random.fold_in(rng, 6)
    for position, parts in shards:
        draws = jnp.exp(jax.random.uniform(jax.random.fold_in(own, position), (parts,), jnp.float32, low / len(shards), high / len(shards)))
        factor_of = factor_of * jnp.repeat(draws, shape[position] // parts).reshape([-1 if axis == position else 1 for axis in range(len(shape))])
    return factor_of


def shared_out(key, own, number, rows, count, top, most, skew):
    ranking = jax.random.permutation(key, count)
    heavy_load, ordinary = load_shares(count, rows * top, most, skew, True), load_shares(count, rows * top, most, skew, False)
    places = jnp.arange(count)

    def named(sizes, turn):
        used = int((sizes > 0).sum())
        fixed = max(1, used // 4)
        moved = fixed + (places - fixed + turn * (used - fixed)) % max(1, count - fixed)
        return jnp.zeros((count,), jnp.int32).at[ranking[jnp.where(places < fixed, places, moved)]].set(jnp.asarray(sizes, jnp.int32))

    sizes = jnp.where(number % 4 == 0, named(heavy_load, number // 4), named(ordinary, number - number // 4 - 1))
    mixed = jax.random.permutation(jax.random.fold_in(own, 3), count)
    donor, taker = mixed[0:count // 2 * 2:2], mixed[1:count // 2 * 2:2]
    slack = jnp.minimum(sizes[donor] - 1, most - sizes[taker]) // 2
    slack = jnp.where((donor == ranking[0]) | (taker == ranking[0]) | (sizes[taker] == 0), 0, jnp.maximum(slack, 0))
    moved = jax.random.randint(jax.random.fold_in(own, 4), (count // 2,), 0, 1 << 20) % (slack + 1)
    sizes = sizes.at[donor].add(-moved).at[taker].add(moved)
    members = jnp.searchsorted(jnp.cumsum(sizes), jnp.arange(rows * top), side="right").astype(jnp.int32)
    listing = members.reshape(top, rows).T
    listing = listing[jax.random.permutation(jax.random.fold_in(own, 1), rows)]
    turn = jax.random.randint(jax.random.fold_in(own, 2), (rows, 1), 0, top)
    return jnp.take_along_axis(listing, (jnp.arange(top)[None, :] + turn) % top, axis=1)


def load_shares(count, total, limit, lean, full):
    portions = [(1 << 20) // math.isqrt(grade ** lean) + 1 for grade in range(1, count + 1)]
    largest = limit if full else min(limit, max(-(-total // count), total * portions[0] // sum(portions)))
    least = 1 if total - largest >= count - 1 else 0
    given, rest = [largest] + [least] * (count - 1), total - largest - least * (count - 1)
    while rest > 0:
        free = [i for i in range(1, count) if given[i] < largest] or [i for i in range(1, count) if given[i] < limit]
        pool, remaining = sum([portions[i] for i in free]), rest
        for i in free:
            more = min(limit - given[i], max(1, remaining * portions[i] // pool), rest)
            given[i] = given[i] + more
            rest = rest - more
    return np.array(given)


def scatter_about(stream_key, shape, spread, limit, pieces=(), kind=jnp.bfloat16):
    values = spread * jax.random.normal(stream_key, shape, jnp.float32)
    if pieces:
        values = values * levels(stream_key, shape, pieces, -0.22, 0.18)
    return jnp.clip(values, -limit, limit).astype(kind)


def setup_inputs(seed: int = 0) -> dict:
    seeds = jax.random.split(jax.random.key(seed), 16)
    query_one = draw_query_one(jax.random.fold_in(seeds[15], 71), 0)
    key_one = draw_key_one(jax.random.fold_in(seeds[15], 71), 0)
    query_two = draw_query_two(jax.random.fold_in(seeds[15], 71), 0)
    key_two = draw_key_two(jax.random.fold_in(seeds[15], 71), 0)
    value = scatter_about(seeds[4], (TOKENS, KV_HEADS * 2 * HEAD), 1.0, 6.0, ((0, 8), (1, 4)))
    lambda_head = jnp.clip(0.3 + 0.5 * jax.random.uniform(seeds[5], (HEADS,), jnp.float32) ** levels(seeds[5], (HEADS,), ((0, 4),), -0.2, 0.2), 0.3, 0.8)
    head_gain = jnp.clip(1.0 + 0.18 * jax.random.normal(seeds[6], (2 * HEAD,), jnp.float32), 0.1, 1.9)
    out_weight = scatter_about(seeds[7], (HEADS * 2 * HEAD, D), (HEADS * 2 * HEAD) ** -0.5, 0.125, ((0, 4),))
    residual = scatter_about(seeds[8], (TOKENS, D), 1.0, 6.0, ((0, 32),))
    norm_gain = jnp.clip(1.0 + 0.18 * jax.random.normal(seeds[9], (D,), jnp.float32), 0.1, 1.9)
    route_expert_keys = jax.random.split(jax.random.fold_in(seeds[10], 1), TOKENS // ROWS_DEV)
    route_expert_turns = jax.random.permutation(jax.random.fold_in(seeds[10], 3), TOKENS // ROWS_DEV)
    route_expert = jax.vmap(lambda own, number: shared_out(jax.random.fold_in(seeds[10], 2), own, number, ROWS_DEV, EXPERTS, TOP, CAP, 2))(route_expert_keys, route_expert_turns).reshape((TOKENS, TOP))
    route_weight = jnp.clip(0.1 + 0.79999997 * jax.random.uniform(seeds[11], (TOKENS, TOP), jnp.float32) ** levels(seeds[11], (TOKENS, TOP), ((0, 32),), -0.2, 0.2), 0.1, 0.9)
    expert_gate = scatter_about(seeds[12], (EXPERTS, D, EXPERT_FF), D ** -0.5, 0.09375, ((0, 8), (2, 4)))
    expert_up = scatter_about(seeds[13], (EXPERTS, D, EXPERT_FF), D ** -0.5, 0.09375, ((0, 8), (2, 4)))
    expert_down = scatter_about(seeds[14], (EXPERTS, EXPERT_FF, D), EXPERT_FF ** -0.5, 0.1875, ((0, 8), (1, 4)))
    return {"query_one": query_one, "key_one": key_one, "query_two": query_two, "key_two": key_two, "value": value, "lambda_head": lambda_head, "head_gain": head_gain, "out_weight": out_weight, "residual": residual, "norm_gain": norm_gain, "route_expert": route_expert, "route_weight": route_weight, "expert_gate": expert_gate, "expert_up": expert_up, "expert_down": expert_down}


def one_map(queries, key_rows, values, allowed):
    scores = jnp.einsum('qhd,khd->hqk', queries, key_rows) * HEAD ** (-0.5)
    scores = jnp.where(allowed[None], scores, -jnp.inf)
    largest = lax.optimization_barrier(jnp.max(scores, axis=-1, keepdims=True))
    weights = jnp.exp(scores - largest)
    totals = lax.optimization_barrier(jnp.sum(weights, axis=-1))
    rounded = lax.optimization_barrier(weights.astype(jnp.bfloat16)).astype(jnp.float32)
    summed = jnp.einsum('hqk,khe->qhe', rounded, values)
    return summed / jnp.transpose(totals)[:, :, None]

def reference(query_one, key_one, query_two, key_two, value, lambda_head, head_gain, out_weight, residual, norm_gain, route_expert, route_weight, expert_gate, expert_up, expert_down):
    per_key = HEADS // KV_HEADS

    def widen(source, columns):
        shaped = source.astype(jnp.float32).reshape(TOKENS, KV_HEADS, columns)
        return jnp.repeat(shaped, per_key, axis=1)
    key_first = widen(key_one, HEAD)
    key_second = widen(key_two, HEAD)
    values = widen(value, 2 * HEAD)
    block_rows = math.gcd(TOKENS, 256)
    positions = jnp.arange(TOKENS, dtype=jnp.int32)

    def attend(block_start):
        first_map = lax.dynamic_slice_in_dim(query_one, block_start, block_rows, 0)
        first_map = first_map.astype(jnp.float32).reshape(block_rows, HEADS, HEAD)
        second_map = lax.dynamic_slice_in_dim(query_two, block_start, block_rows, 0)
        second_map = second_map.astype(jnp.float32).reshape(block_rows, HEADS, HEAD)
        query_pos = block_start + jnp.arange(block_rows, dtype=jnp.int32)
        allowed = positions[None, :] <= query_pos[:, None]
        out_first = one_map(first_map, key_first, values, allowed)
        out_second = one_map(second_map, key_second, values, allowed)
        difference = out_first - lambda_head[None, :, None] * out_second
        scaled = difference * lax.rsqrt(lax.optimization_barrier(jnp.mean(difference * difference, axis=-1, keepdims=True)) + 1e-05) * head_gain
        return scaled.astype(jnp.bfloat16).reshape(block_rows, HEADS * 2 * HEAD)
    starts = jnp.arange(TOKENS // block_rows, dtype=jnp.int32) * block_rows
    attended = lax.map(attend, starts).reshape(TOKENS, HEADS * 2 * HEAD)
    projected = jnp.dot(attended, out_weight, preferred_element_type=jnp.float32)
    summed_in = residual.astype(jnp.float32) + projected
    centered = summed_in - lax.optimization_barrier(jnp.mean(summed_in, axis=-1, keepdims=True))
    variance = lax.optimization_barrier(jnp.mean(centered * centered, axis=-1, keepdims=True))
    normed = (centered * lax.rsqrt(variance + 1e-05) * norm_gain).astype(jnp.bfloat16)
    pair_count = TOKENS * TOP
    chosen = route_expert.reshape(pair_count)
    onehot = (chosen[:, None] == jnp.arange(EXPERTS, dtype=jnp.int32)[None, :]).astype(jnp.int32)
    rank_in = lax.optimization_barrier(jnp.sum((jnp.cumsum(onehot, axis=0) - onehot) * onehot, axis=1))
    most_rows = CAP * (TOKENS // ROWS_DEV)
    slot_table = jnp.full((EXPERTS, most_rows), pair_count, jnp.int32)
    slot_table = slot_table.at[chosen, rank_in].set(jnp.arange(pair_count, dtype=jnp.int32))

    def expert(expert_id):
        pair_ids = slot_table[expert_id]
        token_rows = normed[jnp.minimum(pair_ids, pair_count - 1) // TOP]
        gated = jnp.dot(token_rows, expert_gate[expert_id], preferred_element_type=jnp.float32)
        upward = jnp.dot(token_rows, expert_up[expert_id], preferred_element_type=jnp.float32)
        hidden = (jax.nn.silu(gated) * upward).astype(jnp.bfloat16)
        accum = jnp.zeros((most_rows, D), jnp.float32)
        for segment in range(N_TP):
            partial_value = jnp.dot(hidden[:, segment * FF_PART:(segment + 1) * FF_PART], expert_down[expert_id, segment * FF_PART:(segment + 1) * FF_PART], preferred_element_type=jnp.float32)
            accum = accum + lax.optimization_barrier(partial_value.astype(jnp.bfloat16)).astype(jnp.float32)
        return accum.astype(jnp.bfloat16)
    results = lax.map(expert, jnp.arange(EXPERTS, dtype=jnp.int32))
    gathered = jnp.zeros((pair_count + 1, D), jnp.bfloat16)
    gathered = gathered.at[slot_table.reshape(-1)].set(results.reshape(EXPERTS * most_rows, D))
    picked = gathered[:pair_count].reshape(TOKENS, TOP, D).astype(jnp.float32)
    combined = lax.optimization_barrier(jnp.sum(route_weight[:, :, None] * picked, axis=1))
    return (normed.astype(jnp.float32) + combined).astype(jnp.bfloat16)
```

```python
import math

import jax
import jax.numpy as jnp
from jax import lax
from jax.experimental import pallas as pl
from jax.experimental.pallas import tpu as pltpu
from jax.sharding import PartitionSpec as P

HEAD = 128
GROUP = 4


def map_step(carried, query_rows, key_block, value_block, allowed):
    largest, totals, running = carried
    scores = jnp.einsum(
        "qcgd,kcd->cgqk", query_rows, key_block, preferred_element_type=jnp.float32
    ) * HEAD ** (-0.5)
    scores = jnp.where(allowed[None, None], scores, -jnp.inf)
    updated = jnp.maximum(largest, jnp.max(scores, axis=-1))
    weights = jnp.exp(scores - updated[..., None])
    rescale = jnp.exp(largest - updated)
    totals = totals * rescale + jnp.sum(weights, axis=-1)
    added = jnp.einsum(
        "cgqk,kce->qcge",
        weights.astype(jnp.bfloat16),
        value_block,
        preferred_element_type=jnp.float32,
    )
    running = running * jnp.transpose(rescale, (2, 0, 1))[..., None] + added
    return (updated, totals, running)


def finish(carried):
    return carried[2] / jnp.transpose(carried[1], (2, 0, 1))[..., None]


def pairwise():
    experts, tp_count = lax.axis_size("sp"), lax.axis_size("tp")
    return experts in (2, 4, 8) and tp_count in (2, 4, 8)


def swap(array, axis, bit):
    return lax.ppermute(array, axis, [(i, i ^ bit) for i in range(lax.axis_size(axis))])


def gather_keys(key_one, key_two, value):
    count = lax.axis_size("sp")
    place = lax.axis_index("sp").astype(jnp.int32)
    rows = key_one.shape[0]
    widths = (key_one.shape[1], key_two.shape[1], value.shape[1])

    def pack(first, second, third, out):
        out[:, : widths[0]] = first[...]
        out[:, widths[0] : widths[0] + widths[1]] = second[...]
        out[:, widths[0] + widths[1] :] = third[...]

    own = pl.pallas_call(
        pack, out_shape=jax.ShapeDtypeStruct((rows, sum(widths)), key_one.dtype), name="pack"
    )(key_one, key_two, value)
    blocks, sources = [], []
    lane, line = place % 2, place // 2
    for step in range(count // 2):
        block = own
        if step:
            block = lax.ppermute(own, "sp", [(i, i + 2 * step) for i in range(count - 2 * step)])
        blocks += [block, swap(block, "sp", 1)]
        start = jnp.where(line >= step, (line - step) * 2, count)
        sources += [start + lane, start + (1 - lane)]
    return blocks, jnp.stack(sources) * rows


def attend_pairs(query_one, query_two, blocks, starts, offset, lambda_head, head_gain):
    rows, width = query_one.shape
    heads_here = width // HEAD
    kv_here = blocks[0].shape[1] // (4 * HEAD)
    per_key = heads_here // kv_here
    count = len(blocks)

    def kernel(places, lambdas, first_map, second_map, gain, *refs):
        keys, out = refs[:count], refs[count]
        query_pos = places[count] + lax.broadcasted_iota(jnp.int32, (rows, rows), 0)
        within = lax.broadcasted_iota(jnp.int32, (rows, rows), 1)
        allowed = jnp.concatenate(
            [within + places[b] <= query_pos for b in range(count)], axis=1
        )

        def one(queries, head, base):
            kv_head = head // per_key
            query_rows = queries[:, head * HEAD : (head + 1) * HEAD]
            scores = jnp.concatenate(
                [
                    lax.dot_general(
                        query_rows,
                        key[:, base + kv_head * HEAD : base + (kv_head + 1) * HEAD],
                        (((1,), (1,)), ((), ())),
                        preferred_element_type=jnp.float32,
                    )
                    for key in keys
                ],
                axis=1,
            ) * HEAD ** (-0.5)
            scores = jnp.where(allowed, scores, -jnp.inf)
            weights = jnp.exp(scores - jnp.max(scores, axis=1, keepdims=True))
            totals = jnp.sum(weights, axis=1, keepdims=True)
            rounded = weights.astype(jnp.bfloat16)
            left = 2 * kv_here * HEAD + kv_head * 2 * HEAD
            summed = jnp.zeros((rows, 2 * HEAD), jnp.float32)
            for b, key in enumerate(keys):
                summed = summed + jnp.dot(
                    rounded[:, b * rows : (b + 1) * rows],
                    key[:, left : left + 2 * HEAD],
                    preferred_element_type=jnp.float32,
                )
            return summed / totals

        for head in range(heads_here):
            difference = one(first_map, head, 0) - lambdas[head] * one(
                second_map, head, kv_here * HEAD
            )
            square = jnp.mean(difference * difference, axis=1, keepdims=True)
            scaled = difference * lax.rsqrt(square + 1e-05) * gain[...]
            out[:, head * 2 * HEAD : (head + 1) * 2 * HEAD] = scaled.astype(jnp.bfloat16)

    scalars = pl.BlockSpec(memory_space=pltpu.SMEM)
    whole = pl.BlockSpec(memory_space=pltpu.VMEM)
    places = jnp.concatenate([starts, jnp.reshape(offset, (1,)).astype(jnp.int32)])
    return pl.pallas_call(
        kernel,
        out_shape=jax.ShapeDtypeStruct((rows, heads_here * 2 * HEAD), jnp.bfloat16),
        in_specs=[scalars, scalars] + [whole] * (3 + count),
        out_specs=whole,
        name="attend",
    )(places, lambda_head, query_one, query_two, head_gain[None, :], *blocks)


def bits_of(count):
    return [1 << i for i in range(count.bit_length() - 1)]


def reduce_over(blocks, lowest=1):
    for bit in bits_of(lax.axis_size("tp")):
        if bit < lowest:
            continue
        going = [j for j in blocks if j & bit]
        sent = jnp.concatenate([blocks[j].astype(jnp.bfloat16) for j in going], axis=0)
        came = jnp.split(swap(sent, "tp", bit), len(going), axis=0)
        blocks = {
            j ^ bit: blocks[j ^ bit].astype(jnp.float32) + part.astype(jnp.float32)
            for j, part in zip(going, came)
        }
    return blocks[0]


def gather_over(block):
    blocks = {0: block}
    for bit in reversed(bits_of(lax.axis_size("tp"))):
        for j in list(blocks):
            blocks[j ^ bit] = swap(blocks[j], "tp", bit)
    return blocks


def expert_pairs(pieces, weights):
    gate, up, down = weights
    model_width, hidden_width = gate.shape
    count, rows = len(pieces), pieces[0].shape[0]
    total = count * rows
    steps = 2 if model_width % 256 == 0 else 1
    depth = model_width // steps

    def kernel(*refs):
        parts, (gate_ref, up_ref, down_ref, staying, going) = refs[:count], refs[count : count + 5]
        gated, upward, hidden = refs[count + 5 :]
        step = pl.program_id(0)

        @pl.when(step < steps)
        def _():
            token_rows = jnp.concatenate([part[...] for part in parts], axis=0)
            first = jnp.dot(token_rows, gate_ref[...], preferred_element_type=jnp.float32)
            second = jnp.dot(token_rows, up_ref[...], preferred_element_type=jnp.float32)

            @pl.when(step == 0)
            def _():
                gated[...] = first
                upward[...] = second

            @pl.when(step > 0)
            def _():
                gated[...] += first
                upward[...] += second

        @pl.when(step == steps - 1)
        def _():
            hidden[...] = (jax.nn.silu(gated[...]) * upward[...]).astype(jnp.bfloat16)

        @pl.when(step >= steps)
        def _():
            result = jnp.dot(hidden[...], down_ref[...], preferred_element_type=jnp.float32)
            result = result.astype(jnp.bfloat16)
            staying[...] = result[: total // 2]
            going[...] = result[total // 2 :]

    def early(step):
        return jnp.minimum(step, steps - 1)

    def late(step):
        return jnp.maximum(step - steps, 0)

    half = jax.ShapeDtypeStruct((total // 2, model_width), jnp.bfloat16)
    return pl.pallas_call(
        kernel,
        grid=(2 * steps,),
        in_specs=[pl.BlockSpec((rows, depth), lambda i: (0, early(i)))] * count
        + [pl.BlockSpec((depth, hidden_width), lambda i: (early(i), 0))] * 2
        + [pl.BlockSpec((hidden_width, depth), lambda i: (0, late(i)))],
        out_specs=[pl.BlockSpec((total // 2, depth), lambda i: (0, late(i)))] * 2,
        out_shape=[half, half],
        scratch_shapes=[
            pltpu.VMEM((total, hidden_width), jnp.float32),
            pltpu.VMEM((total, hidden_width), jnp.float32),
            pltpu.VMEM((total, hidden_width), jnp.bfloat16),
        ],
        cost_estimate=pl.CostEstimate(
            flops=6 * total * model_width * hidden_width,
            transcendentals=total * hidden_width,
            bytes_accessed=6 * model_width * hidden_width + 4 * total * model_width,
        ),
        name="expert",
    )(*pieces, gate, up, down)


def reduce_rows(attended, out_weight, own_rows):
    tp_count = lax.axis_size("tp")
    if not pairwise():
        return lax.psum_scatter(
            jnp.dot(attended, out_weight, preferred_element_type=jnp.float32).astype(jnp.bfloat16),
            "tp",
            scatter_dimension=0,
            tiled=True,
        ).astype(jnp.float32)
    place = lax.axis_index("tp")
    ordered = jnp.concatenate(
        [
            lax.dynamic_slice_in_dim(attended, (place ^ j) * own_rows, own_rows, 0)
            for j in range(tp_count)
        ],
        axis=0,
    )
    partial_rows = jnp.dot(ordered, out_weight, preferred_element_type=jnp.float32)
    partial_rows = partial_rows.astype(jnp.bfloat16)
    return reduce_over(dict(enumerate(jnp.split(partial_rows, tp_count, axis=0))))


def run_expert(token_rows, weights):
    gated = jnp.dot(token_rows, weights[0], preferred_element_type=jnp.float32)
    upward = jnp.dot(token_rows, weights[1], preferred_element_type=jnp.float32)
    hidden = (jax.nn.silu(gated) * upward).astype(jnp.bfloat16)
    return jnp.dot(hidden, weights[2], preferred_element_type=jnp.float32).astype(jnp.bfloat16)


def exchange_pairs(placed, normed, weights, experts, capacity):
    outgoing = jnp.einsum("rp,rd->pd", placed, normed, preferred_element_type=jnp.float32)
    outgoing = jnp.split(outgoing.astype(jnp.bfloat16), experts, axis=0)
    arrived = [outgoing[0]] + [swap(outgoing[d], "sp", d) for d in range(1, experts)]
    tp_count = lax.axis_size("tp")
    returned = []
    group = min(GROUP, experts)
    for first in range(0, experts, group):
        blocks = gather_over(jnp.concatenate(arrived[first : first + group], axis=0))
        even, odd = list(range(0, tp_count, 2)), list(range(1, tp_count, 2))
        staying, going = expert_pairs([blocks[j] for j in even + odd], weights)
        came = swap(going, "tp", 1)
        kept = jnp.split(staying.astype(jnp.float32) + came.astype(jnp.float32), len(even), axis=0)
        summed = reduce_over(dict(zip(even, kept)), 2)
        for d, part in enumerate(jnp.split(summed.astype(jnp.bfloat16), group, axis=0), first):
            returned.append(swap(part, "sp", d) if d else part)
    return jnp.concatenate(returned, axis=0)


def exchange_all(placed, normed, weights, experts, capacity):
    model_width = normed.shape[1]
    tp_count = lax.axis_size("tp")
    outgoing = jnp.einsum("rp,rd->pd", placed, normed, preferred_element_type=jnp.float32)
    outgoing = outgoing.astype(jnp.bfloat16).reshape(experts, capacity, model_width)
    arrived = lax.all_to_all(outgoing, "sp", split_axis=0, concat_axis=0, tiled=True)
    token_rows = lax.all_gather(arrived, "tp", axis=0, tiled=True).reshape(-1, model_width)
    partial_value = run_expert(token_rows, weights).reshape(tp_count, -1, model_width)
    summed = lax.psum_scatter(partial_value, "tp", scatter_dimension=0, tiled=True)
    summed = summed.reshape(experts, capacity, model_width)
    returned = lax.all_to_all(summed, "sp", split_axis=0, concat_axis=0, tiled=True)
    return returned.reshape(experts * capacity, model_width)


def on_device(
    query_one,
    key_one,
    query_two,
    key_two,
    value,
    lambda_head,
    head_gain,
    out_weight,
    residual,
    norm_gain,
    route_expert,
    route_weight,
    expert_gate,
    expert_up,
    expert_down,
):
    local_tokens = query_one.shape[0]
    heads_here = lambda_head.shape[0]
    kv_here = key_one.shape[1] // HEAD
    per_key = heads_here // kv_here
    offset = lax.axis_index("sp") * local_tokens
    first_queries = query_one.reshape(local_tokens, kv_here, per_key, HEAD)
    second_queries = query_two.reshape(local_tokens, kv_here, per_key, HEAD)
    query_pos = offset + jnp.arange(local_tokens, dtype=jnp.int32)

    def initial():
        return (
            jnp.full((kv_here, per_key, local_tokens), -1e30, jnp.float32),
            jnp.zeros((kv_here, per_key, local_tokens), jnp.float32),
            jnp.zeros((local_tokens, kv_here, per_key, 2 * HEAD), jnp.float32),
        )

    def attend_all():
        carried = (initial(), initial())
        key_first = lax.all_gather(key_one, "sp", axis=0, tiled=True)
        key_second = lax.all_gather(key_two, "sp", axis=0, tiled=True)
        value_rows = lax.all_gather(value, "sp", axis=0, tiled=True)
        length = key_first.shape[0]
        key_width = math.gcd(length, 1024)

        def attend_block(carried, first_block, second_block, value_block, key_pos):
            width = first_block.shape[0]
            first_block = first_block.reshape(width, kv_here, HEAD)
            second_block = second_block.reshape(width, kv_here, HEAD)
            value_block = value_block.reshape(width, kv_here, 2 * HEAD)
            allowed = key_pos[None, :] <= query_pos[:, None]
            return (
                map_step(carried[0], first_queries, first_block, value_block, allowed),
                map_step(carried[1], second_queries, second_block, value_block, allowed),
            )

        def advance(block_index, carried):
            block_start = block_index * key_width

            def attend(carried):
                first_block = lax.dynamic_slice_in_dim(key_first, block_start, key_width, 0)
                second_block = lax.dynamic_slice_in_dim(key_second, block_start, key_width, 0)
                value_block = lax.dynamic_slice_in_dim(value_rows, block_start, key_width, 0)
                key_pos = block_start + jnp.arange(key_width, dtype=jnp.int32)
                return attend_block(carried, first_block, second_block, value_block, key_pos)

            def unchanged(carried):
                return carried

            return lax.cond(block_start <= offset + local_tokens - 1, attend, unchanged, carried)

        state_one, state_two = lax.fori_loop(0, length // key_width, advance, carried)
        difference = finish(state_one) - lambda_head.reshape(kv_here, per_key)[
            None, :, :, None
        ] * finish(state_two)
        scaled = (
            difference
            * lax.rsqrt(jnp.mean(difference * difference, axis=-1, keepdims=True) + 1e-05)
            * head_gain
        )
        return scaled.astype(jnp.bfloat16).reshape(local_tokens, heads_here * 2 * HEAD)

    if pairwise():
        blocks, starts = gather_keys(key_one, key_two, value)
        attended = attend_pairs(query_one, query_two, blocks, starts, offset, lambda_head, head_gain)
    else:
        attended = attend_all()
    own_rows = residual.shape[0]
    projected = reduce_rows(attended, out_weight, own_rows)
    summed_in = residual.astype(jnp.float32) + projected
    centered = summed_in - jnp.mean(summed_in, axis=-1, keepdims=True)
    variance = jnp.mean(centered * centered, axis=-1, keepdims=True)
    normed = (centered * lax.rsqrt(variance + 1e-05) * norm_gain).astype(jnp.bfloat16)
    experts = lax.axis_size("sp")
    top_count = route_expert.shape[1]
    capacity = max(2 * own_rows * top_count // experts, 2)
    chosen = route_expert.reshape(own_rows * top_count)
    onehot = (chosen[:, None] == jnp.arange(experts, dtype=jnp.int32)[None, :]).astype(jnp.int32)
    slot_index = jnp.sum((jnp.cumsum(onehot, axis=0) - onehot) * onehot, axis=1)
    if pairwise():
        chosen = chosen ^ lax.axis_index("sp").astype(jnp.int32)
    target = chosen * capacity + slot_index
    matches = target[:, None] == jnp.arange(experts * capacity, dtype=jnp.int32)[None, :]
    matches = matches.reshape(own_rows, top_count, experts * capacity)
    placed = jnp.any(matches, axis=1).astype(jnp.bfloat16)
    mixing = jnp.sum(jnp.where(matches, route_weight[:, :, None], 0.0), axis=1)
    weights = (expert_gate[0], expert_up[0], expert_down[0])
    exchange = exchange_pairs if pairwise() else exchange_all
    returned = exchange(placed, normed, weights, experts, capacity)
    coarse = lax.reduce_precision(mixing, 8, 7)
    fine = (mixing - coarse).astype(jnp.bfloat16)
    mixing = jnp.concatenate([coarse.astype(jnp.bfloat16), fine], axis=0)
    combined = jnp.dot(mixing, returned, preferred_element_type=jnp.float32)
    combined = combined[:own_rows] + combined[own_rows:]
    return (normed.astype(jnp.float32) + combined).astype(jnp.bfloat16)


def solution(mesh):
    in_specs = (
        P("sp", "tp"),
        P("sp", "tp"),
        P("sp", "tp"),
        P("sp", "tp"),
        P("sp", "tp"),
        P("tp"),
        P(),
        P("tp", None),
        P(("sp", "tp"), None),
        P(),
        P(("sp", "tp"), None),
        P(("sp", "tp"), None),
        P("sp", None, "tp"),
        P("sp", None, "tp"),
        P("sp", "tp", None),
    )
    out_specs = P(("sp", "tp"), None)
    return jax.shard_map(
        on_device, mesh=mesh, in_specs=in_specs, out_specs=out_specs, check_vma=False
    )
```
